512 devices in a mesh: sp: 32 (over z, core), tp: 16 (over y, x).
Axes of the slice: x: 4, y: 4, z: 16, core: 2. Of those that a mesh axis runs over, the one named last changes fastest.
Arguments:
- outer_gate: bfloat16 [8192, 1024], P('sp', 'tp'), may hold values from -6 to 6
- inner_gate: bfloat16 [8192, 1024], P('sp', 'tp'), may hold values from -6 to 6
- values: bfloat16 [8192, 1024], P('sp', 'tp'), may hold values from -6 to 6
- conv_taps: bfloat16 [3, 1024], P(None, 'tp'), may hold values from -3.5 to 3.5
- document: int32 [8192], P('sp'), may hold values from 0 to 15, never falling along the last dimension, each value on 1 to 1024 neighbouring positions
- mix_proj: bfloat16 [1024, 2048], P('tp'), may hold values from -0.1875 to 0.1875
- stream: bfloat16 [8192, 2048], P('sp'), may hold values from -6 to 6
- norm_gain: float32 [2048], replicated, may hold values from 0.1 to 1.9
- routes: int32 [8192, 2], P('sp'), may hold values from 0 to 31, all different within a row; in each aligned block of 256 rows (0 to 255, 256 to 511, ...) at most 24 rows name the same one
- route_weight: float32 [8192, 2], P('sp'), may hold values from 0.25 to 1
- w_gate: bfloat16 [32, 2048, 4096], P('sp', None, 'tp'), may hold values from -0.125 to 0.125
- w_up: bfloat16 [32, 2048, 4096], P('sp', None, 'tp'), may hold values from -0.125 to 0.125
- w_down: bfloat16 [32, 4096, 2048], P('sp', 'tp'), may hold values from -0.09375 to 0.09375
Outputs:
- mixed: bfloat16 [8192, 2048], P('sp', 'tp')
The draws below stay inside these ranges and needn't reach their ends.
Inputs may be any that keep to these rules, and one draw needn't show every extreme that they name: Document numbers never fall along the sequence; each document holds 1 to 1024 consecutive tokens and one holds exactly that many. `routes`: each token names 2 different experts. Among the 256 tokens of one sp index no expert is named by more than 24 tokens, and in some sp index's tokens an expert is named by exactly 24.
All inputs are finite; a program needn't handle non-finite values.
Results may differ from the reference program's by a relative error of at most 0.014.
Values may be sent and summed in bfloat16 or wider, within the bound.
A program may use at most 64 MiB of HBM per device.

```python
import math
import jax
import jax.numpy as jnp
import numpy as np
from jax import lax

D = 2048
DC = 1024
FFE = 4096
TOP = 2
TAPS = 3
T_SP = 256
TOKENS = 8192
EXPERTS = 32
CAP = 24
N_SP = 32
N_TP = 16


def shard_levels(stream_key, shape, shards, smallest, high):
    gain, own = 1.0, jax.random.fold_in(stream_key, 6)
    for dim, shards_of in shards:
        heights = jnp.exp(jax.random.uniform(jax.random.fold_in(own, dim), (shards_of,), jnp.float32, smallest / len(shards), high / len(shards)))
        gain = gain * jnp.repeat(heights, shape[dim] // shards_of).reshape([-1 if axis == dim else 1 for axis in range(len(shape))])
    return gain


def split_up(amount, total, most, slope):
    weights = [(1 << 20) // math.isqrt(standing ** slope) + 1 for standing in range(2, amount + 1)]
    spare, holding = total - most - (amount - 1), [1] * (amount - 1)
    while spare > 0:
        free = [i for i in range(amount - 1) if holding[i] < most]
        pool, remaining = sum([weights[i] for i in free]), spare
        for i in free:
            extra = min(most - holding[i], max(1, remaining * weights[i] // pool), spare)
            holding[i] = holding[i] + extra
            spare = spare - extra
    return np.array([most] + holding)


def ragged(stream_key, number_of, total, most, slope):
    if number_of == 2:
        one = jax.random.randint(stream_key, (), max(1, total - most), min(most, total - 1) + 1)
        return jnp.stack([one, total - one])
    lengths = jnp.asarray(split_up(number_of, total, most, slope), jnp.int32)
    pairs = (number_of - 1) // 2
    source_of, sink = lengths[1:1 + 2 * pairs:2], lengths[2:2 + 2 * pairs:2]
    slack = jnp.minimum(source_of - 1, most - sink)
    moved = jax.random.randint(jax.random.fold_in(stream_key, 1), (pairs,), 0, 1 << 20) % (slack + 1)
    lengths = lengths.at[1:1 + 2 * pairs:2].set(source_of - moved).at[2:2 + 2 * pairs:2].set(sink + moved)
    return lengths[jax.random.permutation(jax.random.fold_in(stream_key, 2), number_of)]


def assign_block(stream_key, own, number, rows, count, top, most, slope):
    ranking = jax.random.permutation(stream_key, count)
    packed, usual = load_shares(count, rows * top, most, slope, True), load_shares(count, rows * top, most, slope, False)
    places = jnp.arange(count)

    def named(lengths, turn):
        used = int((lengths > 0).sum())
        fixed = max(1, used // 4)
        moved = fixed + (places - fixed + turn * (used - fixed)) % max(1, count - fixed)
        return jnp.zeros((count,), jnp.int32).at[ranking[jnp.where(places < fixed, places, moved)]].set(jnp.asarray(lengths, jnp.int32))

    lengths = jnp.where(number % 4 == 0, named(packed, number // 4), named(usual, number - number // 4 - 1))
    mixed = jax.random.permutation(jax.random.fold_in(own, 3), count)
    source_of, taker = mixed[0:count // 2 * 2:2], mixed[1:count // 2 * 2:2]
    margin = jnp.minimum(lengths[source_of] - 1, most - lengths[taker]) // 2
    margin = jnp.where((source_of == ranking[0]) | (taker == ranking[0]) | (lengths[taker] == 0), 0, jnp.maximum(margin, 0))
    moved = jax.random.randint(jax.random.fold_in(own, 4), (count // 2,), 0, 1 << 20) % (margin + 1)
    lengths = lengths.at[source_of].add(-moved).at[taker].add(moved)
    items = jnp.searchsorted(jnp.cumsum(lengths), jnp.arange(rows * top), side="right").astype(jnp.int32)
    listing = items.reshape(top, rows).T
    listing = listing[jax.random.permutation(jax.random.fold_in(own, 1), rows)]
    turn = jax.random.randint(jax.random.fold_in(own, 2), (rows, 1), 0, top)
    return jnp.take_along_axis(listing, (jnp.arange(top)[None, :] + turn) % top, axis=1)


def load_shares(amount, total, bound, lean, full):
    weights = [(1 << 20) // math.isqrt(rank ** lean) + 1 for rank in range(1, amount + 1)]
    largest = bound if full else min(bound, max(-(-total // amount), total * weights[0] // sum(weights)))
    least = 1 if total - largest >= amount - 1 else 0
    counts, rest = [largest] + [least] * (amount - 1), total - largest - least * (amount - 1)
    while rest > 0:
        candidates = [i for i in range(1, amount) if counts[i] < largest] or [i for i in range(1, amount) if counts[i] < bound]
        pool, budget = sum([weights[i] for i in candidates]), rest
        for i in candidates:
            extra = min(bound - counts[i], max(1, budget * weights[i] // pool), rest)
            counts[i] = counts[i] + extra
            rest = rest - extra
    return np.array(counts)


def centred(stream_key, extent, deviation, reach, cuts=(), kind=jnp.bfloat16):
    factor_of = shard_levels(stream_key, extent, cuts, -0.22, 0.18) if cuts else 1.0
    drawn = jax.random.normal(stream_key, extent, jnp.float32) * deviation * factor_of
    return jnp.minimum(jnp.maximum(drawn, -reach), reach).astype(kind)


def setup_inputs(seed: int = 0) -> dict:
    key_list = jax.random.split(jax.random.key(seed), 14)
    outer_gate = centred(key_list[0], (TOKENS, DC), 1.0, 6.0, ((0, 32), (1, 16)))
    inner_gate = centred(key_list[1], (TOKENS, DC), 1.0, 6.0, ((0, 32), (1, 16)))
    values = centred(key_list[2], (TOKENS, DC), 1.0, 6.0, ((0, 32), (1, 16)))
    conv_taps = centred(key_list[3], (TAPS, DC), TAPS ** -0.5, 3.5, ((1, 16),))
    document = jnp.searchsorted(jnp.cumsum(ragged(key_list[4], N_SP // 2, TOKENS, 4 * T_SP, 1)), jnp.arange(TOKENS), side="right").astype(jnp.int32)
    mix_proj = centred(key_list[5], (DC, D), DC ** -0.5, 0.1875, ((0, 16),))
    stream = centred(key_list[6], (TOKENS, D), 1.0, 6.0, ((0, 32),))
    norm_gain = jnp.clip(1.0 + 0.18 * jax.random.normal(key_list[7], (D,), jnp.float32), 0.1, 1.9)
    routes_keys = jax.random.split(jax.random.fold_in(key_list[8], 1), TOKENS // T_SP)
    routes_turns = jax.random.permutation(jax.random.fold_in(key_list[8], 3), TOKENS // T_SP)
    routes = jax.vmap(lambda own, number: assign_block(jax.random.fold_in(key_list[8], 2), own, number, T_SP, EXPERTS, TOP, CAP, 2))(routes_keys, routes_turns).reshape((TOKENS, TOP))
    route_weight = jnp.clip(0.25 + 0.75 * jax.random.uniform(key_list[9], (TOKENS, TOP), jnp.float32) ** shard_levels(key_list[9], (TOKENS, TOP), ((0, 32),), -0.2, 0.2), 0.25, 1.0)
    w_gate = centred(key_list[10], (EXPERTS, D, FFE), D ** -0.5, 0.125, ((0, 32), (2, 16)))
    w_up = centred(key_list[11], (EXPERTS, D, FFE), D ** -0.5, 0.125, ((0, 32), (2, 16)))
    w_down = centred(key_list[12], (EXPERTS, FFE, D), FFE ** -0.5, 0.09375, ((0, 32), (1, 16)))
    return {"outer_gate": outer_gate, "inner_gate": inner_gate, "values": values, "conv_taps": conv_taps, "document": document, "mix_proj": mix_proj, "stream": stream, "norm_gain": norm_gain, "routes": routes, "route_weight": route_weight, "w_gate": w_gate, "w_up": w_up, "w_down": w_down}


def rounded(value):
    held = lax.optimization_barrier(value.astype(jnp.bfloat16))
    return held.astype(jnp.float32)

def reference(outer_gate, inner_gate, values, conv_taps, document, mix_proj, stream, norm_gain, routes, route_weight, w_gate, w_up, w_down):
    length = stream.shape[0]
    product = inner_gate.astype(jnp.float32) * values.astype(jnp.float32)
    kernel = conv_taps.astype(jnp.float32)
    conv = kernel[2] * product
    for back in (1, 2):
        shifted = jnp.pad(product, ((back, 0), (0, 0)))[:length]
        earlier = jnp.pad(document, (back, 0), constant_values=-1)[:length]
        same = (earlier == document)[:, None]
        conv = conv + kernel[2 - back] * jnp.where(same, shifted, 0.0)
    gated = (outer_gate.astype(jnp.float32) * conv).astype(jnp.bfloat16)
    group_width = DC // N_TP
    branch = jnp.zeros((length, D), jnp.float32)
    for group in range(N_TP):
        lower = group * group_width
        partial_value = jnp.dot(gated[:, lower:lower + group_width], mix_proj[lower:lower + group_width], preferred_element_type=jnp.float32)
        branch = branch + rounded(partial_value)
    hidden_state = stream.astype(jnp.float32) + branch
    scale = lax.rsqrt(lax.optimization_barrier(jnp.mean(hidden_state * hidden_state, axis=-1, keepdims=True)) + 1e-06)
    normed = (hidden_state * scale * norm_gain).astype(jnp.bfloat16)
    flat_expert = routes.reshape(-1).astype(jnp.int32)
    count = flat_expert.shape[0]
    flat_token = jnp.arange(count, dtype=jnp.int32) // TOP
    flat_weight = route_weight.reshape(-1)
    order_key = jnp.arange(count, dtype=jnp.int32)
    limit = N_SP * CAP
    hidden_width = FFE // N_TP

    def per_expert(carry, expert):
        keyed = jnp.where(flat_expert == expert, order_key, count)
        chosen = jnp.argsort(keyed, stable=True)[:limit].astype(jnp.int32)
        valid = jnp.take(keyed, chosen) < count
        token_index = jnp.take(flat_token, chosen)
        taken = jnp.take(normed, token_index, axis=0)
        gate = jnp.dot(taken, w_gate[expert], preferred_element_type=jnp.float32)
        upper = jnp.dot(taken, w_up[expert], preferred_element_type=jnp.float32)
        act = (jax.nn.silu(gate) * upper).astype(jnp.bfloat16)
        down = w_down[expert]
        total = jnp.zeros((limit, D), jnp.float32)
        for group in range(N_TP):
            lower = group * hidden_width
            partial_value = jnp.dot(act[:, lower:lower + hidden_width], down[lower:lower + hidden_width], preferred_element_type=jnp.float32)
            total = total + rounded(partial_value)
        expert_out = rounded(total)
        weight = jnp.where(valid, jnp.take(flat_weight, chosen), 0.0)
        carry = carry.at[token_index].add(weight[:, None] * expert_out)
        return (carry, None)
    combined, _ = lax.scan(per_expert, jnp.zeros((length, D), jnp.float32), jnp.arange(EXPERTS, dtype=jnp.int32))
    return (hidden_state + combined).astype(jnp.bfloat16)
```

```python
import jax
import jax.numpy as jnp
from jax import lax
from jax.experimental import pallas as pl
from jax.experimental.pallas import tpu as pltpu
from jax.sharding import PartitionSpec as P

MESH = pl.DeviceIdType.MESH
F32 = jnp.float32
BF16 = jnp.bfloat16

NZ = 16
NS = 32
CAP = 24
W = 128
CHUNKS = 4
BLOCKS = 8
ROWS = BLOCKS * CAP

ORDER = (0, 1, 15, 2, 14, 3, 13, 4, 12, 5, 11, 6, 10, 7, 9, 8)
PLACE = {r: i for i, r in enumerate(ORDER)}

NT = (((1,), (1,)), ((), ()))


def kernel(
    og_ref, ig_ref, vv_ref, taps_ref, doc_ref, mix_hbm, stream_hbm, gain_ref, routes_ref, rw_ref, wg_hbm, wu_hbm, wd_hbm,
    out_ref,
    mix, stream, wg, wu, wd, hsend, hrecv, mbuf, blk, gbuf, hid, dmat, dt0, dt1, wcol, sent, x_all, lhs, p_all, rb0, rb1, rb2, q_all, f_all, back,
    lsem, hs, hr, ms, mr, gs, gr, zs, zr, as_, ar, rs, rr, bs, br,
):
    s = lax.axis_index("sp")
    t = lax.axis_index("tp")
    z, c = s // 2, s % 2
    y, x = t // 4, t % 4

    def plane(yy, xx):
        return (s, yy * 4 + xx)

    def along_z(r, dc):
        return (z + r + NZ) % NZ * 2 + (c + dc) % 2

    barrier = pltpu.get_barrier_semaphore()
    for d in range(1, 16):
        pl.semaphore_signal(barrier, inc=1, device_id=(s, (t + d) % 16), device_id_type=MESH)
    for d in range(1, NS):
        pl.semaphore_signal(barrier, inc=1, device_id=((s + d) % NS, t), device_id_type=MESH)

    loads = [
        pltpu.make_async_copy(mix_hbm, mix, lsem.at[0]),
        pltpu.make_async_copy(stream_hbm.at[:, pl.ds(pl.multiple_of(t * W, W), W)], stream, lsem.at[1]),
        pltpu.make_async_copy(wg_hbm, wg, lsem.at[2]),
        pltpu.make_async_copy(wu_hbm, wu, lsem.at[3]),
        pltpu.make_async_copy(wd_hbm, wd, lsem.at[4]),
    ]
    for load in loads:
        load.start()

    started = []

    def remote(src, dst, ssem, rsem, device):
        copy = pltpu.make_async_remote_copy(
            src_ref=src, dst_ref=dst, send_sem=ssem, recv_sem=rsem, device_id=device, device_id_type=MESH
        )
        copy.start()
        started.append(copy)
        return copy

    product = ig_ref[...].astype(F32) * vv_ref[...].astype(F32)
    doc = jnp.broadcast_to(doc_ref[...].astype(F32), (8, 256))
    hsend[0:64, :] = product[:, 128:]
    hsend[64:72, :] = doc[:, 128:]
    loads[0].wait()
    pl.semaphore_wait(barrier, 15 + NS - 1)

    halo = remote(hsend, hrecv, hs.at[0], hr.at[0], ((s + 1) % NS, t))
    mixes = []
    for d in range(1, 16):
        j = (t + d) % 16
        mixes.append(
            remote(mix.at[:, pl.ds(pl.multiple_of(j * W, W), W)], mbuf.at[t], ms.at[d], mr.at[d], (s, j))
        )
    mbuf[t] = mix[:, pl.ds(pl.multiple_of(t * W, W), W)]

    eye = (lax.broadcasted_iota(jnp.int32, (64, 64), 0) == lax.broadcasted_iota(jnp.int32, (64, 64), 1)).astype(BF16)
    kernel_taps = lax.dot_general(eye, taps_ref[...], NT, preferred_element_type=F32)

    halo.wait_recv()
    before = hrecv[0:64, :]
    doc_before = jnp.where(s == 0, -1.0, hrecv[64:72, :])
    long = jnp.concatenate([before, product], axis=1)
    long_doc = jnp.concatenate([doc_before, doc], axis=1)
    conv = kernel_taps[:, 2:3] * product
    for step in (1, 2):
        shifted = pltpu.roll(long, step, 1)[:, 128:]
        same = (pltpu.roll(long_doc, step, 1)[:, 128:] == doc)[0:1, :]
        conv = conv + kernel_taps[:, 2 - step : 3 - step] * jnp.where(same, shifted, 0.0)
    gated = og_ref[...].astype(F32) * conv
    folded = jnp.concatenate([gated[:, :128], gated[:, 128:]], axis=0)
    gbuf[t] = folded.T.astype(BF16)
    gathers = []
    for d in range(1, 16):
        gathers.append(remote(gbuf.at[t], gbuf.at[t], gs.at[d], gr.at[d], (s, (t + d) % 16)))

    expert = lax.broadcasted_iota(jnp.int32, (NS, 256), 0)
    first = (routes_ref[0:1, :] == expert).astype(F32)
    second = (routes_ref[1:2, :] == expert).astype(F32)
    used = first + second
    earlier = (lax.broadcasted_iota(jnp.int32, (256, 256), 0) < lax.broadcasted_iota(jnp.int32, (256, 256), 1)).astype(BF16)
    rank = jnp.dot(used.astype(BF16), earlier, preferred_element_type=F32)
    ranked = jnp.where(used > 0.0, rank, -1.0)
    slot = lax.broadcasted_iota(jnp.int32, (CAP, 256), 0).astype(F32)
    for e in range(0, NS, 2):
        pair = [(jnp.broadcast_to(ranked[i : i + 1, :], (CAP, 256)) == slot).astype(F32) for i in (e, e + 1)]
        dmat[e * CAP : (e + 2) * CAP, :] = jnp.concatenate(pair, axis=0).astype(BF16)
    place = expert.astype(F32) * CAP + rank
    rows = [jnp.sum(first * place, axis=0, keepdims=True), jnp.sum(second * place, axis=0, keepdims=True), rw_ref[0:1, :], rw_ref[1:2, :]]
    wcol[...] = jnp.concatenate([*rows, jnp.zeros((124, 256), F32)], axis=0).T
    lane = lax.broadcasted_iota(jnp.int32, (256, NS * CAP), 1).astype(F32)
    dt0[...] = (wcol[:, 0:1] == lane).astype(F32).astype(BF16)
    dt1[...] = (wcol[:, 1:2] == lane).astype(F32).astype(BF16)

    blk[...] = jnp.zeros_like(blk)
    for copy in mixes:
        copy.wait_recv()
    for j in range(16):
        part = mbuf[j]
        blk[128 * j : 128 * j + 64, 0:128] = part
        blk[128 * j + 64 : 128 * j + 128, 128:256] = part
    loads[1].wait()
    for copy in gathers:
        copy.wait_recv()
    branch = jnp.dot(jnp.concatenate([gbuf[j] for j in range(16)], axis=1), blk[...], preferred_element_type=F32)
    hid[0:128, :] = stream[0:128, :].astype(F32) + branch[:, 0:128]
    hid[128:256, :] = stream[128:256, :].astype(F32) + branch[:, 128:256]
    scaled = (hid[...] * gain_ref[pl.ds(t, 1), :]).astype(BF16)
    sent[...] = jnp.dot(dmat[...], scaled, preferred_element_type=F32).reshape(NS, CAP, W).astype(BF16)

    x_all[0, y, x, 0] = sent[s]
    arrivals = {}
    for i, r in enumerate(ORDER):
        for dc in range(2):
            if r == 0 and dc == 0:
                continue
            e = along_z(-r, dc)
            arrivals[2 * i + dc] = remote(
                sent.at[e], x_all.at[i // 4, y, x, i % 4 * 2 + dc], zs.at[2 * i + dc], zr.at[2 * i + dc], (e, t)
            )
    for load in loads[2:]:
        load.wait()

    def span(col, start, size):
        return pl.ds(4 * col + start, size)

    def by_first(col, ref, k, f, start=0, size=4):
        return ref.at[k, :, f, span(col, start, size)] if col == 0 else ref.at[k, f, :, span(col, start, size)]

    def by_second(col, ref, k, g, start=0, size=4):
        fs = pl.ds(start, size)
        return ref.at[k, g, fs, span(col, 0, 4)] if col == 0 else ref.at[k, fs, g, span(col, 0, 4)]

    first_of = (x, y)
    second_of = (y, x)

    def on_first(col, f):
        return plane(y, f) if col == 0 else plane(f, x)

    def on_second(col, g):
        return plane(g, x) if col == 0 else plane(y, g)

    inv_gain = 1.0 / (gain_ref[...] * gain_ref[...])
    pending = {}

    def gather_first(k):
        for b in range(BLOCKS):
            if k or b:
                arrivals[BLOCKS * k + b].wait_recv()
        out = []
        for col in range(2):
            own = x_all.at[k, y, x, span(col, 0, 4)]
            for d in (1, 3, 2):
                i = 3 * col + d - 1
                out.append(remote(own, own, as_.at[k, i], ar.at[k, i], on_first(col, (first_of[col] + d) % 4)))
        pending["first", k] = out

    def gather_second(k):
        for copy in pending["first", k]:
            copy.wait_recv()
        out = []
        for col in range(2):
            g = second_of[col]
            for way, d in enumerate((1, 3)):
                i = 6 + 2 * col + way
                ref = by_second(col, x_all, k, g)
                out.append(remote(ref, ref, as_.at[k, i], ar.at[k, i], on_second(col, (g + d) % 4)))
        pending["second", k] = out

    def gather_third(k):
        for copy in pending["second", k]:
            copy.wait_recv()
        out = []
        for col in range(2):
            g = second_of[col]
            for way, d in enumerate((1, 3)):
                i = 10 + 2 * col + way
                ref = by_second(col, x_all, k, (g + 4 - d) % 4, 2 * way, 2)
                out.append(remote(ref, ref, as_.at[k, i], ar.at[k, i], on_second(col, (g + d) % 4)))
        pending["third", k] = out

    def experts(k):
        for copy in pending["third", k]:
            copy.wait_recv()
        squares = jnp.zeros((ROWS, W), F32)
        for j in range(16):
            part = x_all[k, j // 4, j % 4].astype(F32).reshape(ROWS, W)
            squares = squares + part * part * inv_gain[j : j + 1, :]
            lhs[:, W * j : W * (j + 1)] = part.astype(BF16)
        scale = lax.rsqrt(jnp.sum(squares, axis=1, keepdims=True) / 2048.0 + 1e-06)
        gate = jnp.dot(lhs[...], wg[...], preferred_element_type=F32) * scale
        upper = jnp.dot(lhs[...], wu[...], preferred_element_type=F32) * scale
        act = (gate / (1.0 + jnp.exp(-gate)) * upper).astype(BF16)
        for yy in range(4):
            partial = jnp.dot(act, wd[:, 512 * yy : 512 * (yy + 1)], preferred_element_type=F32)
            for xx in range(4):
                p_all[k, yy, xx] = partial[:, W * xx : W * (xx + 1)].reshape(BLOCKS, CAP, W).astype(BF16)
        out = []
        for col in range(2):
            f = first_of[col]
            for way, d in enumerate((1, 3)):
                i = 2 * col + way
                out.append(
                    remote(
                        by_first(col, p_all, k, (f + 2) % 4, 2 * way, 2), rb0.at[k, col, way],
                        rs.at[k, i], rr.at[k, i], on_first(col, (f + d) % 4),
                    )
                )
        pending["opposite", k] = out

    def reduce_first(k):
        for copy in pending["opposite", k]:
            copy.wait_recv()
        out = []
        for col in range(2):
            f = first_of[col]
            for way, d in enumerate((1, 3)):
                i = 4 + 2 * col + way
                other = (f + d) % 4
                half = by_first(col, p_all, k, other, 2 * way, 2)
                half[...] = (half[...].astype(F32) + rb0[k, col, way].astype(F32)).astype(BF16)
                out.append(
                    remote(by_first(col, p_all, k, other), rb1.at[k, col, way], rs.at[k, i], rr.at[k, i], on_first(col, other))
                )
        pending["nearby", k] = out

    def reduce_second(k):
        for copy in pending["nearby", k]:
            copy.wait_recv()
        out = []
        for col in range(2):
            f, g = first_of[col], second_of[col]
            total = by_first(col, p_all, k, f)[...].astype(F32) + rb1[k, col, 0].astype(F32) + rb1[k, col, 1].astype(F32)
            q_all[k, col] = total.astype(BF16)
            for d in (1, 3, 2):
                i = 8 + 3 * col + d - 1
                other = (g + d) % 4
                out.append(remote(q_all.at[k, col, other], rb2.at[k, col, d - 1], rs.at[k, i], rr.at[k, i], on_second(col, other)))
        pending["last", k] = out

    returns = []

    def give_back(k):
        for copy in pending["last", k]:
            copy.wait_recv()
        for col in range(2):
            total = q_all[k, col, second_of[col]].astype(F32)
            for d in range(3):
                total = total + rb2[k, col, d].astype(F32)
            f_all[k, 4 * col : 4 * col + 4] = total.astype(BF16)
        for b in range(BLOCKS):
            i = BLOCKS * k + b
            if i == 0:
                back[s] = f_all[0, 0]
                continue
            home = along_z(ORDER[i // 2], i % 2)
            returns.append(remote(f_all.at[k, b], back.at[s], bs.at[i], br.at[i], (home, t)))

    stages = (gather_first, gather_second, gather_third, experts, reduce_first, reduce_second, give_back)
    for step in range(CHUNKS + len(stages) - 1):
        for number, stage in enumerate(stages):
            if 0 <= step - number < CHUNKS:
                stage(step - number)

    for copy in returns:
        copy.wait_recv()
    landed = back[...].astype(F32).reshape(NS * CAP, W).astype(BF16)
    one = jnp.dot(dt0[...], landed, preferred_element_type=F32)
    two = jnp.dot(dt1[...], landed, preferred_element_type=F32)
    out_ref[...] = (hid[...] + (wcol[:, 2:3] * one + wcol[:, 3:4] * two)).astype(BF16)
    for copy in started:
        copy.wait_send()


def body(outer_gate, inner_gate, values, conv_taps, document, mix_proj, stream, norm_gain, routes, route_weight, w_gate, w_up, w_down):
    vmem = pl.BlockSpec(memory_space=pltpu.VMEM)
    hbm = pl.BlockSpec(memory_space=pl.ANY)
    dma = pltpu.SemaphoreType.DMA
    scratch = [
        pltpu.VMEM((64, 2048), BF16),
        pltpu.VMEM((256, W), BF16),
        pltpu.VMEM((2048, 256), BF16),
        pltpu.VMEM((2048, 256), BF16),
        pltpu.VMEM((256, 2048), BF16),
        pltpu.VMEM((72, 128), F32),
        pltpu.VMEM((72, 128), F32),
        pltpu.VMEM((16, 64, W), BF16),
        pltpu.VMEM((2048, 256), BF16),
        pltpu.VMEM((16, 128, 128), BF16),
        pltpu.VMEM((256, W), F32),
        pltpu.VMEM((NS * CAP, 256), BF16),
        pltpu.VMEM((256, NS * CAP), BF16),
        pltpu.VMEM((256, NS * CAP), BF16),
        pltpu.VMEM((256, 128), F32),
        pltpu.VMEM((NS, CAP, W), BF16),
        pltpu.VMEM((CHUNKS, 4, 4, BLOCKS, CAP, W), BF16),
        pltpu.VMEM((ROWS, 2048), BF16),
        pltpu.VMEM((CHUNKS, 4, 4, BLOCKS, CAP, W), BF16),
        pltpu.VMEM((CHUNKS, 2, 2, 4, 2, CAP, W), BF16),
        pltpu.VMEM((CHUNKS, 2, 2, 4, 4, CAP, W), BF16),
        pltpu.VMEM((CHUNKS, 2, 3, 4, CAP, W), BF16),
        pltpu.VMEM((CHUNKS, 2, 4, 4, CAP, W), BF16),
        pltpu.VMEM((CHUNKS, BLOCKS, CAP, W), BF16),
        pltpu.VMEM((NS, CAP, W), BF16),
        dma((5,)),
        dma((1,)), dma((1,)),
        dma((16,)), dma((16,)),
        dma((16,)), dma((16,)),
        dma((NS,)), dma((NS,)),
        dma((CHUNKS, 14)), dma((CHUNKS, 14)),
        dma((CHUNKS, 14)), dma((CHUNKS, 14)),
        dma((NS,)), dma((NS,)),
    ]
    return pl.pallas_call(
        kernel,
        out_shape=jax.ShapeDtypeStruct((256, W), BF16),
        in_specs=[vmem, vmem, vmem, vmem, vmem, hbm, hbm, vmem, vmem, vmem, hbm, hbm, hbm],
        out_specs=vmem,
        scratch_shapes=scratch,
        compiler_params=pltpu.CompilerParams(collective_id=0, has_side_effects=True, vmem_limit_bytes=60 * 2**20),
        name="block",
    )(
        outer_gate.T, inner_gate.T, values.T, conv_taps, document.reshape(1, 256), mix_proj, stream, norm_gain.reshape(16, 128),
        routes.T, route_weight.T, w_gate[0], w_up[0], w_down[0],
    )


def solution(mesh):
    placed = (
        P("sp", "tp"), P("sp", "tp"), P("sp", "tp"), P(None, "tp"), P("sp"), P("tp", None), P("sp", None), P(),
        P("sp", None), P("sp", None), P("sp", None, "tp"), P("sp", None, "tp"), P("sp", "tp", None),
    )
    return jax.shard_map(body, mesh=mesh, in_specs=placed, out_specs=P("sp", "tp"), check_vma=False)
```

```python
import jax
import jax.numpy as jnp
from jax import lax
from jax.experimental import pallas as pl
from jax.experimental.pallas import tpu as pltpu
from jax.sharding import PartitionSpec as P

MESH = pl.DeviceIdType.MESH
F32 = jnp.float32
BF16 = jnp.bfloat16

NZ = 16
NS = 32
CAP = 24
W = 128
CHUNKS = 8
BLOCKS = NS // CHUNKS
HALF = BLOCKS // 2
PART = HALF // 2
ROWS = BLOCKS * CAP

ORDER = (0, 1, 14, 3, 13, 4, 9, 8, 10, 7, 11, 6, 12, 5, 15, 2)

SCHEDULE = ((0, 0), (0, 1), (0, 2), (1, 0), (1, 1), (1, 2), (0, 3), (2, 0), (0, 4), (0, 7), (0, 5), (2, 1), (2, 2), (0, 6), (1, 3), (1, 4), (1, 5), (1, 7), (2, 3), (3, 2), (2, 4), (1, 6), (2, 5), (3, 1), (2, 7), (3, 3), (4, 2), (3, 4), (2, 6), (3, 0), (3, 5), (3, 7), (4, 3), (4, 4), (3, 6), (4, 7), (5, 3), (4, 5), (5, 4), (4, 6), (4, 1), (5, 5), (4, 0), (6, 3), (6, 4), (5, 6), (5, 2), (5, 7), (5, 1), (6, 5), (5, 0), (6, 6), (6, 2), (6, 1), (6, 7), (6, 0))

NT = (((1,), (1,)), ((), ()))


def kernel(
    og_hbm, ig_hbm, vv_hbm, taps_hbm, doc_hbm, mix_hbm, stream_hbm, gain_hbm, routes_hbm, rw_hbm, wg_hbm, wu_hbm, wd_hbm,
    out_ref,
    gates, taps_ref, doc_ref, gain_ref, routes_ref, rw_ref, mix, stream, wg, wu, wd, hsend, hrecv, mbuf, blk, gbuf, hid, dmat, dt0, dt1, wcol, sent, x_all, lhs, p_all, rb0, rb1, rb2, q_all, f_all, back,
    lsem, hs, hr, ms, mr, gs, gr, zs, zr, ss, sr, bs, br,
):
    s = lax.axis_index("sp")
    t = lax.axis_index("tp")
    z, c = s // 2, s % 2
    y, x = t // 4, t % 4

    def plane(yy, xx):
        return (s, yy * 4 + xx)

    def along_z(r, dc):
        return (z + r + NZ) % NZ * 2 + (c + dc) % 2

    barrier = pltpu.get_barrier_semaphore()
    for d in range(1, 16):
        pl.semaphore_signal(barrier, inc=1, device_id=(s, (t + d) % 16), device_id_type=MESH)
    for d in range(1, NS):
        pl.semaphore_signal(barrier, inc=1, device_id=((s + d) % NS, t), device_id_type=MESH)

    pairs = (
        (ig_hbm, gates.at[0]), (vv_hbm, gates.at[1]), (doc_hbm, doc_ref), (mix_hbm, mix), (og_hbm, gates.at[2]), (taps_hbm, taps_ref),
        (routes_hbm, routes_ref), (rw_hbm, rw_ref), (gain_hbm, gain_ref),
        (stream_hbm.at[:, pl.ds(pl.multiple_of(t * W, W), W)], stream), (wg_hbm, wg), (wu_hbm, wu), (wd_hbm, wd),
    )
    loads = [pltpu.make_async_copy(src, dst, lsem.at[i]) for i, (src, dst) in enumerate(pairs)]
    for load in loads:
        load.start()

    def wait_for(ref, sem):
        pltpu.make_async_copy(ref, ref, sem).wait()

    def remote(src, dst, ssem, rsem, device):
        copy = pltpu.make_async_remote_copy(
            src_ref=src, dst_ref=dst, send_sem=ssem, recv_sem=rsem, device_id=device, device_id_type=MESH
        )
        copy.start()

    for load in loads[:3]:
        load.wait()
    product = gates[0].astype(F32) * gates[1].astype(F32)
    doc = jnp.broadcast_to(doc_ref[...].astype(F32), (8, 256))
    hsend[0:64, :] = product[:, 128:]
    hsend[64:72, :] = doc[:, 128:]
    loads[3].wait()
    pl.semaphore_wait(barrier, 15 + NS - 1)

    remote(hsend, hrecv, hs.at[0], hr.at[0], ((s + 1) % NS, t))
    for d in range(1, 16):
        j = (t + d) % 16
        remote(mix.at[:, pl.ds(pl.multiple_of(j * W, W), W)], mbuf.at[t], ms.at[0], mr.at[0], (s, j))
    mbuf[t] = mix[:, pl.ds(pl.multiple_of(t * W, W), W)]

    eye = (lax.broadcasted_iota(jnp.int32, (64, 64), 0) == lax.broadcasted_iota(jnp.int32, (64, 64), 1)).astype(BF16)
    for load in loads[4:]:
        load.wait()
    kernel_taps = lax.dot_general(eye, taps_ref[...], NT, preferred_element_type=F32)

    wait_for(hrecv, hr.at[0])
    before = hrecv[0:64, :]
    doc_before = jnp.where(s == 0, -1.0, hrecv[64:72, :])
    long = jnp.concatenate([before, product], axis=1)
    long_doc = jnp.concatenate([doc_before, doc], axis=1)
    conv = kernel_taps[:, 2:3] * product
    for step in (1, 2):
        shifted = pltpu.roll(long, step, 1)[:, 128:]
        same = (pltpu.roll(long_doc, step, 1)[:, 128:] == doc)[0:1, :]
        conv = conv + kernel_taps[:, 2 - step : 3 - step] * jnp.where(same, shifted, 0.0)
    gated = gates[2].astype(F32) * conv
    folded = jnp.concatenate([gated[:, :128], gated[:, 128:]], axis=0)
    gbuf[t] = folded.T.astype(BF16)
    for d in range(1, 16):
        remote(gbuf.at[t], gbuf.at[t], gs.at[0], gr.at[0], (s, (t + d) % 16))

    expert = lax.broadcasted_iota(jnp.int32, (NS, 256), 0)
    first = (routes_ref[0:1, :] == expert).astype(F32)
    second = (routes_ref[1:2, :] == expert).astype(F32)
    used = first + second
    earlier = (lax.broadcasted_iota(jnp.int32, (256, 256), 0) < lax.broadcasted_iota(jnp.int32, (256, 256), 1)).astype(BF16)
    rank = jnp.dot(used.astype(BF16), earlier, preferred_element_type=F32)
    ranked = jnp.where(used > 0.0, rank, -1.0)
    slot = lax.broadcasted_iota(jnp.int32, (CAP, 256), 0).astype(F32)
    for e in range(0, NS, 2):
        pair = [(jnp.broadcast_to(ranked[i : i + 1, :], (CAP, 256)) == slot).astype(F32) for i in (e, e + 1)]
        dmat[e * CAP : (e + 2) * CAP, :] = jnp.concatenate(pair, axis=0).astype(BF16)
    place = expert.astype(F32) * CAP + rank
    rows = [jnp.sum(first * place, axis=0, keepdims=True), jnp.sum(second * place, axis=0, keepdims=True), rw_ref[0:1, :], rw_ref[1:2, :]]
    wcol[...] = jnp.concatenate([*rows, jnp.zeros((124, 256), F32)], axis=0).T
    lane = lax.broadcasted_iota(jnp.int32, (256, NS * CAP), 1).astype(F32)
    dt0[...] = (wcol[:, 0:1] == lane).astype(F32).astype(BF16)
    dt1[...] = (wcol[:, 1:2] == lane).astype(F32).astype(BF16)

    blk[...] = jnp.zeros_like(blk)
    wait_for(mbuf.at[0:15], mr.at[0])
    for j in range(16):
        part = mbuf[j]
        blk[128 * j : 128 * j + 64, 0:128] = part
        blk[128 * j + 64 : 128 * j + 128, 128:256] = part
    wait_for(gbuf.at[0:15], gr.at[0])
    branch = jnp.dot(jnp.concatenate([gbuf[j] for j in range(16)], axis=1), blk[...], preferred_element_type=F32)
    hid[0:128, :] = stream[0:128, :].astype(F32) + branch[:, 0:128]
    hid[128:256, :] = stream[128:256, :].astype(F32) + branch[:, 128:256]
    scaled = (hid[...] * gain_ref[pl.ds(t, 1), :]).astype(BF16)
    sent[...] = jnp.dot(dmat[...], scaled, preferred_element_type=F32).reshape(NS, CAP, W).astype(BF16)

    x_all[0, y, x, 0] = sent[s]
    for i, r in enumerate(ORDER):
        for dc in range(2):
            if r == 0 and dc == 0:
                continue
            e = along_z(-r, dc)
            remote(sent.at[e], x_all.at[2 * i // BLOCKS, y, x, 2 * i % BLOCKS + dc], zs.at[0], zr.at[2 * i // BLOCKS], (e, t))

    def span(col, start, size):
        return pl.ds(HALF * col + start, size)

    def by_first(col, ref, k, f, start=0, size=HALF):
        return ref.at[k, :, f, span(col, start, size)] if col == 0 else ref.at[k, f, :, span(col, start, size)]

    def by_second(col, ref, k, g, start=0, size=4):
        fs = pl.ds(start, size)
        return ref.at[k, g, fs, span(col, 0, HALF)] if col == 0 else ref.at[k, fs, g, span(col, 0, HALF)]

    first_of = (x, y)
    second_of = (y, x)

    def on_first(col, f):
        return plane(y, f) if col == 0 else plane(f, x)

    def on_second(col, g):
        return plane(g, x) if col == 0 else plane(y, g)

    inv_gain = 1.0 / (gain_ref[...] * gain_ref[...])

    def gather_first(k):
        wait_for(sent.at[0 : BLOCKS if k else BLOCKS - 1], zr.at[k])
        for col in range(2):
            own = x_all.at[k, y, x, span(col, 0, HALF)]
            for d in (1, 3, 2):
                remote(own, own, ss.at[0], sr.at[0, k], on_first(col, (first_of[col] + d) % 4))

    def gather_second(k):
        wait_for(x_all.at[0, 0, 0:3], sr.at[0, k])
        for col in range(2):
            g = second_of[col]
            for d in (1, 3):
                ref = by_second(col, x_all, k, g)
                remote(ref, ref, ss.at[1], sr.at[1, k], on_second(col, (g + d) % 4))

    def gather_third(k):
        wait_for(x_all.at[0, 0:2], sr.at[1, k])
        for col in range(2):
            g = second_of[col]
            for way, d in enumerate((1, 3)):
                ref = by_second(col, x_all, k, (g + 4 - d) % 4, 2 * way, 2)
                remote(ref, ref, ss.at[2], sr.at[2, k], on_second(col, (g + d) % 4))

    def experts(k):
        wait_for(x_all.at[0, 0], sr.at[2, k])
        squares = jnp.zeros((ROWS, W), F32)
        for j in range(16):
            part = x_all[k, j // 4, j % 4].astype(F32).reshape(ROWS, W)
            squares = squares + part * part * inv_gain[j : j + 1, :]
            lhs[:, W * j : W * (j + 1)] = part.astype(BF16)
        scale = lax.rsqrt(jnp.sum(squares, axis=1, keepdims=True) / 2048.0 + 1e-06)
        gate = jnp.dot(lhs[...], wg[...], preferred_element_type=F32) * scale
        upper = jnp.dot(lhs[...], wu[...], preferred_element_type=F32) * scale
        act = (gate / (1.0 + jnp.exp(-gate)) * upper).astype(BF16)
        for yy in range(4):
            partial = jnp.dot(act, wd[:, 512 * yy : 512 * (yy + 1)], preferred_element_type=F32)
            for xx in range(4):
                p_all[k, yy, xx] = partial[:, W * xx : W * (xx + 1)].reshape(BLOCKS, CAP, W).astype(BF16)
        for col in range(2):
            f = first_of[col]
            for way, d in enumerate((1, 3)):
                ref = by_first(col, p_all, k, (f + 2) % 4, PART * way, PART)
                remote(ref, rb0.at[k, col, way], ss.at[3], sr.at[3, k], on_first(col, (f + d) % 4))

    def reduce_first(k):
        wait_for(x_all.at[0, 0], sr.at[3, k])
        for col in range(2):
            f = first_of[col]
            for way, d in enumerate((1, 3)):
                other = (f + d) % 4
                half = by_first(col, p_all, k, other, PART * way, PART)
                half[...] = (half[...].astype(F32) + rb0[k, col, way].astype(F32)).astype(BF16)
                remote(by_first(col, p_all, k, other), rb1.at[k, col, way], ss.at[4], sr.at[4, k], on_first(col, other))

    def reduce_second(k):
        wait_for(x_all.at[0, 0:2], sr.at[4, k])
        for col in range(2):
            f, g = first_of[col], second_of[col]
            total = by_first(col, p_all, k, f)[...].astype(F32) + rb1[k, col, 0].astype(F32) + rb1[k, col, 1].astype(F32)
            q_all[k, col] = total.astype(BF16)
            for d in (1, 3, 2):
                other = (g + d) % 4
                remote(q_all.at[k, col, other], rb2.at[k, col, d - 1], ss.at[5], sr.at[5, k], on_second(col, other))

    def give_back(k):
        wait_for(x_all.at[0, 0, 0:3], sr.at[5, k])
        for col in range(2):
            total = q_all[k, col, second_of[col]].astype(F32)
            for d in range(3):
                total = total + rb2[k, col, d].astype(F32)
            f_all[k, HALF * col : HALF * (col + 1)] = total.astype(BF16)
        for b in range(BLOCKS):
            i = BLOCKS * k + b
            if i == 0:
                back[s] = f_all[0, 0]
                continue
            home = along_z(ORDER[i // 2], i % 2)
            remote(f_all.at[k, b], back.at[s], bs.at[0], br.at[0], (home, t))

    stages = (gather_first, gather_second, gather_third, experts, reduce_first, reduce_second, give_back)
    for number, k in SCHEDULE:
        stages[number](k)

    wait_for(sent.at[0:31], br.at[0])
    landed = back[...].astype(F32).reshape(NS * CAP, W).astype(BF16)
    one = jnp.dot(dt0[...], landed, preferred_element_type=F32)
    two = jnp.dot(dt1[...], landed, preferred_element_type=F32)
    out_ref[...] = (hid[...] + (wcol[:, 2:3] * one + wcol[:, 3:4] * two)).astype(BF16)
    wait_for(hrecv, hs.at[0])
    wait_for(mbuf.at[0:15], ms.at[0])
    wait_for(gbuf.at[0:15], gs.at[0])
    wait_for(sent.at[0:31], zs.at[0])
    wait_for(sent.at[0:31], bs.at[0])
    for i, size in enumerate((3, 8, 4, 4, 8, 3)):
        wait_for(x_all.at[:, 0 : max(1, size // 4), 0 : min(size, 4)], ss.at[i])


def body(outer_gate, inner_gate, values, conv_taps, document, mix_proj, stream, norm_gain, routes, route_weight, w_gate, w_up, w_down):
    vmem = pl.BlockSpec(memory_space=pltpu.VMEM)
    hbm = pl.BlockSpec(memory_space=pl.ANY)
    dma = pltpu.SemaphoreType.DMA
    scratch = [
        pltpu.VMEM((3, 64, 256), BF16),
        pltpu.VMEM((3, 64), BF16),
        pltpu.VMEM((1, 256), jnp.int32),
        pltpu.VMEM((16, 128), F32),
        pltpu.VMEM((2, 256), jnp.int32),
        pltpu.VMEM((2, 256), F32),
        pltpu.VMEM((64, 2048), BF16),
        pltpu.VMEM((256, W), BF16),
        pltpu.VMEM((2048, 256), BF16),
        pltpu.VMEM((2048, 256), BF16),
        pltpu.VMEM((256, 2048), BF16),
        pltpu.VMEM((72, 128), F32),
        pltpu.VMEM((72, 128), F32),
        pltpu.VMEM((16, 64, W), BF16),
        pltpu.VMEM((2048, 256), BF16),
        pltpu.VMEM((16, 128, 128), BF16),
        pltpu.VMEM((256, W), F32),
        pltpu.VMEM((NS * CAP, 256), BF16),
        pltpu.VMEM((256, NS * CAP), BF16),
        pltpu.VMEM((256, NS * CAP), BF16),
        pltpu.VMEM((256, 128), F32),
        pltpu.VMEM((NS, CAP, W), BF16),
        pltpu.VMEM((CHUNKS, 4, 4, BLOCKS, CAP, W), BF16),
        pltpu.VMEM((ROWS, 2048), BF16),
        pltpu.VMEM((CHUNKS, 4, 4, BLOCKS, CAP, W), BF16),
        pltpu.VMEM((CHUNKS, 2, 2, 4, PART, CAP, W), BF16),
        pltpu.VMEM((CHUNKS, 2, 2, 4, HALF, CAP, W), BF16),
        pltpu.VMEM((CHUNKS, 2, 3, HALF, CAP, W), BF16),
        pltpu.VMEM((CHUNKS, 2, 4, HALF, CAP, W), BF16),
        pltpu.VMEM((CHUNKS, BLOCKS, CAP, W), BF16),
        pltpu.VMEM((NS, CAP, W), BF16),
        dma((13,)),
        dma((1,)), dma((1,)),
        dma((1,)), dma((1,)),
        dma((1,)), dma((1,)),
        dma((1,)), dma((CHUNKS,)),
        dma((6,)), dma((6, CHUNKS)),
        dma((1,)), dma((1,)),
    ]
    return pl.pallas_call(
        kernel,
        out_shape=jax.ShapeDtypeStruct((256, W), BF16),
        in_specs=[hbm] * 13,
        out_specs=vmem,
        scratch_shapes=scratch,
        compiler_params=pltpu.CompilerParams(collective_id=0, has_side_effects=True, vmem_limit_bytes=60 * 2**20),
        name="block",
    )(
        outer_gate.T, inner_gate.T, values.T, conv_taps, document.reshape(1, 256), mix_proj, stream, norm_gain.reshape(16, 128),
        routes.T, route_weight.T, w_gate[0], w_up[0], w_down[0],
    )


def solution(mesh):
    placed = (
        P("sp", "tp"), P("sp", "tp"), P("sp", "tp"), P(None, "tp"), P("sp"), P("tp", None), P("sp", None), P(),
        P("sp", None), P("sp", None), P("sp", None, "tp"), P("sp", None, "tp"), P("sp", "tp", None),
    )
    return jax.shard_map(body, mesh=mesh, in_specs=placed, out_specs=P("sp", "tp"), check_vma=False)
```

```python
import jax
import jax.numpy as jnp
from jax import lax
from jax.experimental import pallas as pl
from jax.experimental.pallas import tpu as pltpu
from jax.sharding import PartitionSpec as P

MESH = pl.DeviceIdType.MESH
F32 = jnp.float32
BF16 = jnp.bfloat16

NZ = 16
NS = 32
CAP = 24
W = 128
CHUNKS = 8
BLOCKS = NS // CHUNKS
HALF = BLOCKS // 2
PART = HALF // 2
ROWS = BLOCKS * CAP

ORDER = (0, 1, 14, 3, 13, 4, 9, 8, 10, 7, 11, 6, 12, 5, 15, 2)

SCHEDULE = ((0, 0), (0, 1), (1, 0), (0, 2), (1, 1), (0, 3), (0, 7), (0, 5), (0, 6), (0, 4), (1, 2), (2, 1), (1, 3), (1, 5), (1, 4), (1, 6), (2, 3), (3, 1), (2, 5), (2, 0), (2, 4), (1, 7), (2, 6), (3, 3), (2, 2), (4, 1), (3, 5), (3, 4), (2, 7), (4, 3), (3, 6), (3, 2), (4, 5), (4, 4), (5, 3), (5, 1), (3, 7), (4, 6), (3, 0), (5, 4), (4, 2), (5, 5), (6, 3), (4, 7), (5, 6), (6, 1), (4, 0), (6, 4), (5, 2), (6, 5), (5, 7), (5, 0), (6, 6), (6, 2), (6, 7), (6, 0))

NT = (((1,), (1,)), ((), ()))


def kernel(
    og_hbm, ig_hbm, vv_hbm, taps_hbm, doc_hbm, mix_hbm, stream_hbm, gain_hbm, routes_hbm, rw_hbm, wg_hbm, wu_hbm, wd_hbm,
    out_ref,
    gates, taps_ref, doc_ref, gain_ref, routes_ref, rw_ref, mix, stream, wg, wu, wd, hsend, hrecv, mbuf, mother, gfix, blk, gbuf, hid, dmat, dt0, dt1, wcol, sent, x_all, lhs, p_all, rb0, rb1, rb2, q_all, f_all, back,
    lsem, hs, hr, ms, mr, gs, gr, fs, fr, zs, zr, ss, sr, bs, br,
):
    s = lax.axis_index("sp")
    t = lax.axis_index("tp")
    z, c = s // 2, s % 2
    y, x = t // 4, t % 4

    def plane(yy, xx):
        return (s, yy * 4 + xx)

    def along_z(r, dc):
        return (z + r + NZ) % NZ * 2 + (c + dc) % 2

    barrier = pltpu.get_barrier_semaphore()
    for d in range(1, 16):
        pl.semaphore_signal(barrier, inc=1, device_id=(s, (t + d) % 16), device_id_type=MESH)
    for d in range(1, NS):
        pl.semaphore_signal(barrier, inc=1, device_id=((s + d) % NS, t), device_id_type=MESH)

    pairs = (
        (ig_hbm, gates.at[0]), (vv_hbm, gates.at[1]), (doc_hbm, doc_ref), (og_hbm, gates.at[2]), (taps_hbm, taps_ref), (mix_hbm, mix),
        (routes_hbm, routes_ref), (rw_hbm, rw_ref), (gain_hbm, gain_ref),
        (stream_hbm.at[:, pl.ds(pl.multiple_of(t * W, W), W)], stream), (wg_hbm, wg), (wu_hbm, wu), (wd_hbm, wd),
    )
    loads = [pltpu.make_async_copy(src, dst, lsem.at[i]) for i, (src, dst) in enumerate(pairs)]
    for load in loads:
        load.start()

    def wait_for(ref, sem):
        pltpu.make_async_copy(ref, ref, sem).wait()

    def remote(src, dst, ssem, rsem, device):
        copy = pltpu.make_async_remote_copy(
            src_ref=src, dst_ref=dst, send_sem=ssem, recv_sem=rsem, device_id=device, device_id_type=MESH
        )
        copy.start()

    for load in loads[:6]:
        load.wait()
    product = gates[0].astype(F32) * gates[1].astype(F32)
    doc = jnp.broadcast_to(doc_ref[...].astype(F32), (8, 256))
    hsend[0:64, :] = product[:, 128:]
    hsend[64:72, :] = doc[:, 128:]
    eye = (lax.broadcasted_iota(jnp.int32, (64, 64), 0) == lax.broadcasted_iota(jnp.int32, (64, 64), 1)).astype(BF16)
    kernel_taps = lax.dot_general(eye, taps_ref[...], NT, preferred_element_type=F32)

    def convolve(before, doc_before):
        long = jnp.concatenate([before, product], axis=1)
        long_doc = jnp.concatenate([doc_before, doc], axis=1)
        conv = kernel_taps[:, 2:3] * product
        for step in (1, 2):
            shifted = pltpu.roll(long, step, 1)[:, 128:]
            same = (pltpu.roll(long_doc, step, 1)[:, 128:] == doc)[0:1, :]
            conv = conv + kernel_taps[:, 2 - step : 3 - step] * jnp.where(same, shifted, 0.0)
        gated = gates[2].astype(F32) * conv
        return jnp.concatenate([gated[:, :128], gated[:, 128:]], axis=0).T.astype(BF16)

    gbuf[t] = convolve(jnp.zeros((64, 128), F32), jnp.full((8, 128), -1.0, F32))
    pl.semaphore_wait(barrier, 15 + NS - 1)

    remote(hsend, hrecv, hs.at[0], hr.at[0], ((s + 1) % NS, t))
    half_rows = pl.ds(pl.multiple_of(16 * (2 * (z % 2) + c), 16), 16)
    for d in range(1, 16):
        j = (t + d) % 16
        remote(mix.at[half_rows, pl.ds(pl.multiple_of(j * W, W), W)], mbuf.at[t], ms.at[0], mr.at[0], (s, j))
    for d in range(1, 16):
        remote(gbuf.at[t], gbuf.at[t], gs.at[0], gr.at[0], (s, (t + d) % 16))
    mbuf[t] = mix[half_rows, pl.ds(pl.multiple_of(t * W, W), W)]
    for load in loads[6:]:
        load.wait()

    wait_for(hrecv, hr.at[0])
    folded = convolve(hrecv[0:64, :], jnp.where(s == 0, -1.0, hrecv[64:72, :]))
    gfix[t] = folded[0:8, :]
    for d in range(1, 16):
        remote(gfix.at[t], gfix.at[t], fs.at[0], fr.at[0], (s, (t + d) % 16))

    expert = lax.broadcasted_iota(jnp.int32, (NS, 256), 0)
    first = (routes_ref[0:1, :] == expert).astype(F32)
    second = (routes_ref[1:2, :] == expert).astype(F32)
    used = first + second
    earlier = (lax.broadcasted_iota(jnp.int32, (256, 256), 0) < lax.broadcasted_iota(jnp.int32, (256, 256), 1)).astype(BF16)
    rank = jnp.dot(used.astype(BF16), earlier, preferred_element_type=F32)
    ranked = jnp.where(used > 0.0, rank, -1.0)
    slot = lax.broadcasted_iota(jnp.int32, (CAP, 256), 0).astype(F32)
    for e in range(0, NS, 2):
        pair = [(jnp.broadcast_to(ranked[i : i + 1, :], (CAP, 256)) == slot).astype(F32) for i in (e, e + 1)]
        dmat[e * CAP : (e + 2) * CAP, :] = jnp.concatenate(pair, axis=0).astype(BF16)
    place = expert.astype(F32) * CAP + rank
    rows = [jnp.sum(first * place, axis=0, keepdims=True), jnp.sum(second * place, axis=0, keepdims=True), rw_ref[0:1, :], rw_ref[1:2, :]]
    wcol[...] = jnp.concatenate([*rows, jnp.zeros((124, 256), F32)], axis=0).T
    lane = lax.broadcasted_iota(jnp.int32, (256, NS * CAP), 1).astype(F32)
    dt0[...] = (wcol[:, 0:1] == lane).astype(F32).astype(BF16)
    dt1[...] = (wcol[:, 1:2] == lane).astype(F32).astype(BF16)

    blk[...] = jnp.zeros_like(blk)
    wait_for(mbuf.at[0:15], mr.at[0])
    remote(mbuf, mother.at[0], ms.at[1], mr.at[1], (s + 2 - 4 * (z % 2), t))

    def spread(buffer, quarter):
        for j in range(16):
            part = buffer[j]
            blk[pl.ds(pl.multiple_of(128 * j + 16 * quarter, 16), 16), 0:128] = part
            blk[pl.ds(pl.multiple_of(128 * j + 64 + 16 * quarter, 16), 16), 128:256] = part

    odd = z % 2
    spread(mbuf, 2 * odd + c)
    wait_for(mother.at[0], mr.at[1])
    remote(mbuf, mother.at[1], ms.at[2], mr.at[2], (s + 1 - 2 * c, t))
    remote(mother.at[0], mother.at[2], ms.at[3], mr.at[3], (s + 1 - 2 * c, t))
    spread(mother.at[0], 2 - 2 * odd + c)
    wait_for(mother.at[1], mr.at[2])
    spread(mother.at[1], 2 * odd + 1 - c)
    wait_for(mother.at[2], mr.at[3])
    spread(mother.at[2], 3 - 2 * odd - c)
    wait_for(gbuf.at[0:15], gr.at[0])
    branch = jnp.dot(jnp.concatenate([gbuf[j] for j in range(16)], axis=1), blk[...], preferred_element_type=F32)
    hid[8:128, :] = stream[8:128, :].astype(F32) + branch[8:128, 0:128]
    hid[128:256, :] = stream[128:256, :].astype(F32) + branch[:, 128:256]
    wait_for(gfix.at[0:15], fr.at[0])
    fixed = jnp.concatenate([gfix[j].astype(F32) for j in range(16)], axis=1).astype(BF16)
    branch = jnp.dot(fixed, blk[...], preferred_element_type=F32)
    hid[0:8, :] = stream[0:8, :].astype(F32) + branch[:, 0:128]
    scaled = (hid[...] * gain_ref[pl.ds(t, 1), :]).astype(BF16)
    sent[...] = jnp.dot(dmat[...], scaled, preferred_element_type=F32).reshape(NS, CAP, W).astype(BF16)

    x_all[0, y, x, 0] = sent[s]
    for i, r in enumerate(ORDER):
        for dc in range(2):
            if r == 0 and dc == 0:
                continue
            e = along_z(-r, dc)
            remote(sent.at[e], x_all.at[2 * i // BLOCKS, y, x, 2 * i % BLOCKS + dc], zs.at[0], zr.at[2 * i // BLOCKS], (e, t))

    def span(col, start, size):
        return pl.ds(HALF * col + start, size)

    def by_first(col, ref, k, f, start=0, size=HALF):
        return ref.at[k, :, f, span(col, start, size)] if col == 0 else ref.at[k, f, :, span(col, start, size)]

    def by_second(col, ref, k, g, start=0, size=4):
        fs = pl.ds(start, size)
        return ref.at[k, g, fs, span(col, 0, HALF)] if col == 0 else ref.at[k, fs, g, span(col, 0, HALF)]

    first_of = (x, y)
    second_of = (y, x)

    def on_first(col, f):
        return plane(y, f) if col == 0 else plane(f, x)

    def on_second(col, g):
        return plane(g, x) if col == 0 else plane(y, g)

    inv_gain = 1.0 / (gain_ref[...] * gain_ref[...])

    def gather_first(k):
        wait_for(sent.at[0 : BLOCKS if k else BLOCKS - 1], zr.at[k])
        for col in range(2):
            own = x_all.at[k, y, x, span(col, 0, HALF)]
            for d in (1, 3, 2):
                remote(own, own, ss.at[0], sr.at[0, k], on_first(col, (first_of[col] + d) % 4))

    def gather_second(k):
        wait_for(x_all.at[0, 0, 0:3], sr.at[0, k])
        for col in range(2):
            g = second_of[col]
            for d in (1, 3):
                ref = by_second(col, x_all, k, g)
                remote(ref, ref, ss.at[1], sr.at[1, k], on_second(col, (g + d) % 4))

    def gather_third(k):
        wait_for(x_all.at[0, 0:2], sr.at[1, k])
        for col in range(2):
            g = second_of[col]
            for way, d in enumerate((1, 3)):
                ref = by_second(col, x_all, k, (g + 4 - d) % 4, 2 * way, 2)
                remote(ref, ref, ss.at[2], sr.at[2, k], on_second(col, (g + d) % 4))

    def experts(k):
        wait_for(x_all.at[0, 0], sr.at[2, k])
        squares = jnp.zeros((ROWS, W), F32)
        for j in range(16):
            part = x_all[k, j // 4, j % 4].astype(F32).reshape(ROWS, W)
            squares = squares + part * part * inv_gain[j : j + 1, :]
            lhs[:, W * j : W * (j + 1)] = part.astype(BF16)
        scale = lax.rsqrt(jnp.sum(squares, axis=1, keepdims=True) / 2048.0 + 1e-06)
        gate = jnp.dot(lhs[...], wg[...], preferred_element_type=F32) * scale
        upper = jnp.dot(lhs[...], wu[...], preferred_element_type=F32) * scale
        act = (gate / (1.0 + jnp.exp(-gate)) * upper).astype(BF16)
        for yy in range(4):
            partial = jnp.dot(act, wd[:, 512 * yy : 512 * (yy + 1)], preferred_element_type=F32)
            for xx in range(4):
                p_all[k, yy, xx] = partial[:, W * xx : W * (xx + 1)].reshape(BLOCKS, CAP, W).astype(BF16)
        for col in range(2):
            f = first_of[col]
            for way, d in enumerate((1, 3)):
                ref = by_first(col, p_all, k, (f + 2) % 4, PART * way, PART)
                remote(ref, rb0.at[k, col, way], ss.at[3], sr.at[3, k], on_first(col, (f + d) % 4))

    def reduce_first(k):
        wait_for(x_all.at[0, 0], sr.at[3, k])
        for col in range(2):
            f = first_of[col]
            for way, d in enumerate((1, 3)):
                other = (f + d) % 4
                half = by_first(col, p_all, k, other, PART * way, PART)
                half[...] = (half[...].astype(F32) + rb0[k, col, way].astype(F32)).astype(BF16)
                remote(by_first(col, p_all, k, other), rb1.at[k, col, way], ss.at[4], sr.at[4, k], on_first(col, other))

    def reduce_second(k):
        wait_for(x_all.at[0, 0:2], sr.at[4, k])
        for col in range(2):
            f, g = first_of[col], second_of[col]
            total = by_first(col, p_all, k, f)[...].astype(F32) + rb1[k, col, 0].astype(F32) + rb1[k, col, 1].astype(F32)
            q_all[k, col] = total.astype(BF16)
            for d in (1, 3, 2):
                other = (g + d) % 4
                remote(q_all.at[k, col, other], rb2.at[k, col, d - 1], ss.at[5], sr.at[5, k], on_second(col, other))

    def give_back(k):
        wait_for(x_all.at[0, 0, 0:3], sr.at[5, k])
        for col in range(2):
            total = q_all[k, col, second_of[col]].astype(F32)
            for d in range(3):
                total = total + rb2[k, col, d].astype(F32)
            f_all[k, HALF * col : HALF * (col + 1)] = total.astype(BF16)
        for b in range(BLOCKS):
            i = BLOCKS * k + b
            if i == 0:
                back[s] = f_all[0, 0]
                continue
            home = along_z(ORDER[i // 2], i % 2)
            remote(f_all.at[k, b], back.at[s], bs.at[0], br.at[0], (home, t))

    stages = (gather_first, gather_second, gather_third, experts, reduce_first, reduce_second, give_back)
    for number, k in SCHEDULE:
        stages[number](k)

    wait_for(sent.at[0:31], br.at[0])
    landed = back[...].astype(F32).reshape(NS * CAP, W).astype(BF16)
    one = jnp.dot(dt0[...], landed, preferred_element_type=F32)
    two = jnp.dot(dt1[...], landed, preferred_element_type=F32)
    out_ref[...] = (hid[...] + (wcol[:, 2:3] * one + wcol[:, 3:4] * two)).astype(BF16)
    wait_for(hrecv, hs.at[0])
    wait_for(mbuf.at[0:15], ms.at[0])
    for i in range(1, 4):
        wait_for(mbuf, ms.at[i])
    wait_for(gfix.at[0:15], fs.at[0])
    wait_for(gbuf.at[0:15], gs.at[0])
    wait_for(sent.at[0:31], zs.at[0])
    wait_for(sent.at[0:31], bs.at[0])
    for i, size in enumerate((3, 8, 4, 4, 8, 3)):
        wait_for(x_all.at[:, 0 : max(1, size // 4), 0 : min(size, 4)], ss.at[i])


def body(outer_gate, inner_gate, values, conv_taps, document, mix_proj, stream, norm_gain, routes, route_weight, w_gate, w_up, w_down):
    vmem = pl.BlockSpec(memory_space=pltpu.VMEM)
    hbm = pl.BlockSpec(memory_space=pl.ANY)
    dma = pltpu.SemaphoreType.DMA
    scratch = [
        pltpu.VMEM((3, 64, 256), BF16),
        pltpu.VMEM((3, 64), BF16),
        pltpu.VMEM((1, 256), jnp.int32),
        pltpu.VMEM((16, 128), F32),
        pltpu.VMEM((2, 256), jnp.int32),
        pltpu.VMEM((2, 256), F32),
        pltpu.VMEM((64, 2048), BF16),
        pltpu.VMEM((256, W), BF16),
        pltpu.VMEM((2048, 256), BF16),
        pltpu.VMEM((2048, 256), BF16),
        pltpu.VMEM((256, 2048), BF16),
        pltpu.VMEM((72, 128), F32),
        pltpu.VMEM((72, 128), F32),
        pltpu.VMEM((16, 16, W), BF16),
        pltpu.VMEM((3, 16, 16, W), BF16),
        pltpu.VMEM((16, 8, W), BF16),
        pltpu.VMEM((2048, 256), BF16),
        pltpu.VMEM((16, 128, 128), BF16),
        pltpu.VMEM((256, W), F32),
        pltpu.VMEM((NS * CAP, 256), BF16),
        pltpu.VMEM((256, NS * CAP), BF16),
        pltpu.VMEM((256, NS * CAP), BF16),
        pltpu.VMEM((256, 128), F32),
        pltpu.VMEM((NS, CAP, W), BF16),
        pltpu.VMEM((CHUNKS, 4, 4, BLOCKS, CAP, W), BF16),
        pltpu.VMEM((ROWS, 2048), BF16),
        pltpu.VMEM((CHUNKS, 4, 4, BLOCKS, CAP, W), BF16),
        pltpu.VMEM((CHUNKS, 2, 2, 4, PART, CAP, W), BF16),
        pltpu.VMEM((CHUNKS, 2, 2, 4, HALF, CAP, W), BF16),
        pltpu.VMEM((CHUNKS, 2, 3, HALF, CAP, W), BF16),
        pltpu.VMEM((CHUNKS, 2, 4, HALF, CAP, W), BF16),
        pltpu.VMEM((CHUNKS, BLOCKS, CAP, W), BF16),
        pltpu.VMEM((NS, CAP, W), BF16),
        dma((13,)),
        dma((1,)), dma((1,)),
        dma((4,)), dma((4,)),
        dma((1,)), dma((1,)),
        dma((1,)), dma((1,)),
        dma((1,)), dma((CHUNKS,)),
        dma((6,)), dma((6, CHUNKS)),
        dma((1,)), dma((1,)),
    ]
    return pl.pallas_call(
        kernel,
        out_shape=jax.ShapeDtypeStruct((256, W), BF16),
        in_specs=[hbm] * 13,
        out_specs=vmem,
        scratch_shapes=scratch,
        compiler_params=pltpu.CompilerParams(collective_id=0, has_side_effects=True, vmem_limit_bytes=60 * 2**20),
        name="block",
    )(
        outer_gate.T, inner_gate.T, values.T, conv_taps, document.reshape(1, 256), mix_proj, stream, norm_gain.reshape(16, 128),
        routes.T, route_weight.T, w_gate[0], w_up[0], w_down[0],
    )


def solution(mesh):
    placed = (
        P("sp", "tp"), P("sp", "tp"), P("sp", "tp"), P(None, "tp"), P("sp"), P("tp", None), P("sp", None), P(),
        P("sp", None), P("sp", None), P("sp", None, "tp"), P("sp", None, "tp"), P("sp", "tp", None),
    )
    return jax.shard_map(body, mesh=mesh, in_specs=placed, out_specs=P("sp", "tp"), check_vma=False)
```

```python
import jax
import jax.numpy as jnp
from jax import lax
from jax.experimental import pallas as pl
from jax.experimental.pallas import tpu as pltpu
from jax.sharding import PartitionSpec as P

MESH = pl.DeviceIdType.MESH
F32 = jnp.float32
BF16 = jnp.bfloat16

NZ = 16
NS = 32
CAP = 24
W = 128
CHUNKS = 8
BLOCKS = NS // CHUNKS
HALF = BLOCKS // 2
PART = HALF // 2
ROWS = BLOCKS * CAP

ORDER = (0, 1, 14, 3, 13, 4, 9, 8, 10, 7, 11, 6, 12, 5, 15, 2)

SCHEDULE = ((0, 0), (0, 1), (1, 0), (0, 2), (1, 1), (0, 3), (0, 7), (0, 5), (0, 6), (0, 4), (1, 2), (2, 1), (1, 3), (1, 5), (1, 4), (1, 6), (2, 3), (3, 1), (2, 5), (2, 0), (2, 4), (1, 7), (2, 6), (3, 3), (2, 2), (4, 1), (3, 5), (3, 4), (2, 7), (4, 3), (3, 6), (3, 2), (4, 5), (4, 4), (5, 3), (5, 1), (3, 7), (4, 6), (3, 0), (5, 4), (4, 2), (5, 5), (6, 3), (4, 7), (5, 6), (6, 1), (4, 0), (6, 4), (5, 2), (6, 5), (5, 7), (5, 0), (6, 6), (6, 2), (6, 7), (6, 0))

FAR_FIRST = sorted(((dy, dx) for dy in range(4) for dx in range(4) if dy or dx), key=lambda d: -min(d[0], 4 - d[0]) - min(d[1], 4 - d[1]))

NT = (((1,), (1,)), ((), ()))


def kernel(
    og_hbm, ig_hbm, vv_hbm, taps_hbm, doc_hbm, mix_hbm, stream_hbm, gain_hbm, routes_hbm, rw_hbm, wg_hbm, wu_hbm, wd_hbm,
    out_ref,
    gates, taps_ref, doc_ref, gain_ref, routes_ref, rw_ref, mix, stream, wg, wu, wd, hsend, hrecv, mbuf, mother, gfix, blk, gbuf, hid, dmat, dt0, dt1, wcol, sent, x_all, lhs, p_all, rb0, rb1, rb2, q_all, f_all, back,
    lsem, hs, hr, ms, mr, gs, gr, fs, fr, zs, zr, ss, sr, bs, br,
):
    s = lax.axis_index("sp")
    t = lax.axis_index("tp")
    z, c = s // 2, s % 2
    y, x = t // 4, t % 4

    def plane(yy, xx):
        return (s, yy * 4 + xx)

    def along_z(r, dc):
        return (z + r + NZ) % NZ * 2 + (c + dc) % 2

    barrier = pltpu.get_barrier_semaphore()
    for d in range(1, 16):
        pl.semaphore_signal(barrier, inc=1, device_id=(s, (t + d) % 16), device_id_type=MESH)
    for d in range(1, NS):
        pl.semaphore_signal(barrier, inc=1, device_id=((s + d) % NS, t), device_id_type=MESH)

    pairs = (
        (ig_hbm, gates.at[0]), (vv_hbm, gates.at[1]), (doc_hbm, doc_ref), (og_hbm, gates.at[2]), (taps_hbm, taps_ref), (mix_hbm, mix),
        (routes_hbm, routes_ref), (rw_hbm, rw_ref), (gain_hbm, gain_ref),
        (stream_hbm.at[:, pl.ds(pl.multiple_of(t * W, W), W)], stream), (wg_hbm, wg), (wu_hbm, wu), (wd_hbm, wd),
    )
    loads = [pltpu.make_async_copy(src, dst, lsem.at[i]) for i, (src, dst) in enumerate(pairs)]
    for load in loads:
        load.start()

    def wait_for(ref, sem):
        pltpu.make_async_copy(ref, ref, sem).wait()

    def remote(src, dst, ssem, rsem, device):
        copy = pltpu.make_async_remote_copy(
            src_ref=src, dst_ref=dst, send_sem=ssem, recv_sem=rsem, device_id=device, device_id_type=MESH
        )
        copy.start()

    for load in loads[:6]:
        load.wait()
    product = gates[0].astype(F32) * gates[1].astype(F32)
    doc = jnp.broadcast_to(doc_ref[...].astype(F32), (8, 256))
    hsend[0:64, :] = product[:, 128:]
    hsend[64:72, :] = doc[:, 128:]
    eye = (lax.broadcasted_iota(jnp.int32, (64, 64), 0) == lax.broadcasted_iota(jnp.int32, (64, 64), 1)).astype(BF16)
    kernel_taps = lax.dot_general(eye, taps_ref[...], NT, preferred_element_type=F32)

    def convolve(before, doc_before):
        long = jnp.concatenate([before, product], axis=1)
        long_doc = jnp.concatenate([doc_before, doc], axis=1)
        conv = kernel_taps[:, 2:3] * product
        for step in (1, 2):
            shifted = pltpu.roll(long, step, 1)[:, 128:]
            same = (pltpu.roll(long_doc, step, 1)[:, 128:] == doc)[0:1, :]
            conv = conv + kernel_taps[:, 2 - step : 3 - step] * jnp.where(same, shifted, 0.0)
        gated = gates[2].astype(F32) * conv
        return jnp.concatenate([gated[:, :128], gated[:, 128:]], axis=0).T.astype(BF16)

    gbuf[t] = convolve(jnp.zeros((64, 128), F32), jnp.full((8, 128), -1.0, F32))
    pl.semaphore_wait(barrier, 15 + NS - 1)

    remote(hsend, hrecv, hs.at[0], hr.at[0], ((s + 1) % NS, t))
    others = [(y + dy) % 4 * 4 + (x + dx) % 4 for dy, dx in FAR_FIRST]
    half_rows = pl.ds(pl.multiple_of(16 * (2 * (z % 2) + c), 16), 16)
    for j in others:
        remote(mix.at[half_rows, pl.ds(pl.multiple_of(j * W, W), W)], mbuf.at[t], ms.at[0], mr.at[0], (s, j))
    for j in others:
        remote(gbuf.at[t], gbuf.at[t], gs.at[0], gr.at[0], (s, j))
    mbuf[t] = mix[half_rows, pl.ds(pl.multiple_of(t * W, W), W)]
    for load in loads[6:]:
        load.wait()

    wait_for(hrecv, hr.at[0])
    folded = convolve(hrecv[0:64, :], jnp.where(s == 0, -1.0, hrecv[64:72, :]))
    gfix[t] = folded[0:8, :]
    for j in others:
        remote(gfix.at[t], gfix.at[t], fs.at[0], fr.at[0], (s, j))

    expert = lax.broadcasted_iota(jnp.int32, (NS, 256), 0)
    first = (routes_ref[0:1, :] == expert).astype(F32)
    second = (routes_ref[1:2, :] == expert).astype(F32)
    used = first + second
    earlier = (lax.broadcasted_iota(jnp.int32, (256, 256), 0) < lax.broadcasted_iota(jnp.int32, (256, 256), 1)).astype(BF16)
    rank = jnp.dot(used.astype(BF16), earlier, preferred_element_type=F32)
    ranked = jnp.where(used > 0.0, rank, -1.0)
    slot = lax.broadcasted_iota(jnp.int32, (CAP, 256), 0).astype(F32)
    for e in range(0, NS, 2):
        pair = [(jnp.broadcast_to(ranked[i : i + 1, :], (CAP, 256)) == slot).astype(F32) for i in (e, e + 1)]
        dmat[e * CAP : (e + 2) * CAP, :] = jnp.concatenate(pair, axis=0).astype(BF16)
    place = expert.astype(F32) * CAP + rank
    rows = [jnp.sum(first * place, axis=0, keepdims=True), jnp.sum(second * place, axis=0, keepdims=True), rw_ref[0:1, :], rw_ref[1:2, :]]
    wcol[...] = jnp.concatenate([*rows, jnp.zeros((124, 256), F32)], axis=0).T
    lane = lax.broadcasted_iota(jnp.int32, (256, NS * CAP), 1).astype(F32)
    dt0[...] = (wcol[:, 0:1] == lane).astype(F32).astype(BF16)
    dt1[...] = (wcol[:, 1:2] == lane).astype(F32).astype(BF16)

    blk[...] = jnp.zeros_like(blk)
    wait_for(mbuf.at[0:15], mr.at[0])
    remote(mbuf, mother.at[0], ms.at[1], mr.at[1], (s + 2 - 4 * (z % 2), t))

    def spread(buffer, quarter):
        for j in range(16):
            part = buffer[j]
            blk[pl.ds(pl.multiple_of(128 * j + 16 * quarter, 16), 16), 0:128] = part
            blk[pl.ds(pl.multiple_of(128 * j + 64 + 16 * quarter, 16), 16), 128:256] = part

    odd = z % 2
    spread(mbuf, 2 * odd + c)
    wait_for(mother.at[0], mr.at[1])
    remote(mbuf, mother.at[1], ms.at[2], mr.at[2], (s + 1 - 2 * c, t))
    remote(mother.at[0], mother.at[2], ms.at[3], mr.at[3], (s + 1 - 2 * c, t))
    spread(mother.at[0], 2 - 2 * odd + c)
    wait_for(mother.at[1], mr.at[2])
    spread(mother.at[1], 2 * odd + 1 - c)
    wait_for(mother.at[2], mr.at[3])
    spread(mother.at[2], 3 - 2 * odd - c)
    wait_for(gbuf.at[0:15], gr.at[0])
    branch = jnp.dot(jnp.concatenate([gbuf[j] for j in range(16)], axis=1), blk[...], preferred_element_type=F32)
    hid[8:128, :] = stream[8:128, :].astype(F32) + branch[8:128, 0:128]
    hid[128:256, :] = stream[128:256, :].astype(F32) + branch[:, 128:256]
    wait_for(gfix.at[0:15], fr.at[0])
    fixed = jnp.concatenate([gfix[j].astype(F32) for j in range(16)], axis=1).astype(BF16)
    branch = jnp.dot(fixed, blk[...], preferred_element_type=F32)
    hid[0:8, :] = stream[0:8, :].astype(F32) + branch[:, 0:128]
    scaled = (hid[...] * gain_ref[pl.ds(t, 1), :]).astype(BF16)
    sent[...] = jnp.dot(dmat[...], scaled, preferred_element_type=F32).reshape(NS, CAP, W).astype(BF16)

    x_all[0, y, x, 0] = sent[s]
    for i, r in enumerate(ORDER):
        for dc in range(2):
            if r == 0 and dc == 0:
                continue
            e = along_z(-r, dc)
            remote(sent.at[e], x_all.at[2 * i // BLOCKS, y, x, 2 * i % BLOCKS + dc], zs.at[0], zr.at[2 * i // BLOCKS], (e, t))

    def span(col, start, size):
        return pl.ds(HALF * col + start, size)

    def by_first(col, ref, k, f, start=0, size=HALF):
        return ref.at[k, :, f, span(col, start, size)] if col == 0 else ref.at[k, f, :, span(col, start, size)]

    def by_second(col, ref, k, g, start=0, size=4):
        fs = pl.ds(start, size)
        return ref.at[k, g, fs, span(col, 0, HALF)] if col == 0 else ref.at[k, fs, g, span(col, 0, HALF)]

    first_of = (x, y)
    second_of = (y, x)

    def on_first(col, f):
        return plane(y, f) if col == 0 else plane(f, x)

    def on_second(col, g):
        return plane(g, x) if col == 0 else plane(y, g)

    inv_gain = 1.0 / (gain_ref[...] * gain_ref[...])

    def gather_first(k):
        wait_for(sent.at[0 : BLOCKS if k else BLOCKS - 1], zr.at[k])
        for col in range(2):
            own = x_all.at[k, y, x, span(col, 0, HALF)]
            for d in (1, 3, 2):
                remote(own, own, ss.at[0], sr.at[0, k], on_first(col, (first_of[col] + d) % 4))

    def gather_second(k):
        wait_for(x_all.at[0, 0, 0:3], sr.at[0, k])
        for col in range(2):
            g = second_of[col]
            for d in (1, 3):
                ref = by_second(col, x_all, k, g)
                remote(ref, ref, ss.at[1], sr.at[1, k], on_second(col, (g + d) % 4))

    def gather_third(k):
        wait_for(x_all.at[0, 0:2], sr.at[1, k])
        for col in range(2):
            g = second_of[col]
            for way, d in enumerate((1, 3)):
                ref = by_second(col, x_all, k, (g + 4 - d) % 4, 2 * way, 2)
                remote(ref, ref, ss.at[2], sr.at[2, k], on_second(col, (g + d) % 4))

    def experts(k):
        wait_for(x_all.at[0, 0], sr.at[2, k])
        squares = jnp.zeros((ROWS, W), F32)
        for j in range(16):
            part = x_all[k, j // 4, j % 4].astype(F32).reshape(ROWS, W)
            squares = squares + part * part * inv_gain[j : j + 1, :]
            lhs[:, W * j : W * (j + 1)] = part.astype(BF16)
        scale = lax.rsqrt(jnp.sum(squares, axis=1, keepdims=True) / 2048.0 + 1e-06)
        gate = jnp.dot(lhs[...], wg[...], preferred_element_type=F32) * scale
        upper = jnp.dot(lhs[...], wu[...], preferred_element_type=F32) * scale
        act = (gate / (1.0 + jnp.exp(-gate)) * upper).astype(BF16)
        for yy in range(4):
            partial = jnp.dot(act, wd[:, 512 * yy : 512 * (yy + 1)], preferred_element_type=F32)
            for xx in range(4):
                p_all[k, yy, xx] = partial[:, W * xx : W * (xx + 1)].reshape(BLOCKS, CAP, W).astype(BF16)
        for col in range(2):
            f = first_of[col]
            for way, d in enumerate((1, 3)):
                ref = by_first(col, p_all, k, (f + 2) % 4, PART * way, PART)
                remote(ref, rb0.at[k, col, way], ss.at[3], sr.at[3, k], on_first(col, (f + d) % 4))

    def reduce_first(k):
        wait_for(x_all.at[0, 0], sr.at[3, k])
        for col in range(2):
            f = first_of[col]
            for way, d in enumerate((1, 3)):
                other = (f + d) % 4
                half = by_first(col, p_all, k, other, PART * way, PART)
                half[...] = (half[...].astype(F32) + rb0[k, col, way].astype(F32)).astype(BF16)
                remote(by_first(col, p_all, k, other), rb1.at[k, col, way], ss.at[4], sr.at[4, k], on_first(col, other))

    def reduce_second(k):
        wait_for(x_all.at[0, 0:2], sr.at[4, k])
        for col in range(2):
            f, g = first_of[col], second_of[col]
            total = by_first(col, p_all, k, f)[...].astype(F32) + rb1[k, col, 0].astype(F32) + rb1[k, col, 1].astype(F32)
            q_all[k, col] = total.astype(BF16)
            for d in (1, 3, 2):
                other = (g + d) % 4
                remote(q_all.at[k, col, other], rb2.at[k, col, d - 1], ss.at[5], sr.at[5, k], on_second(col, other))

    def give_back(k):
        wait_for(x_all.at[0, 0, 0:3], sr.at[5, k])
        for col in range(2):
            total = q_all[k, col, second_of[col]].astype(F32)
            for d in range(3):
                total = total + rb2[k, col, d].astype(F32)
            f_all[k, HALF * col : HALF * (col + 1)] = total.astype(BF16)
        for b in range(BLOCKS):
            i = BLOCKS * k + b
            if i == 0:
                back[s] = f_all[0, 0]
                continue
            home = along_z(ORDER[i // 2], i % 2)
            remote(f_all.at[k, b], back.at[s], bs.at[0], br.at[0], (home, t))

    stages = (gather_first, gather_second, gather_third, experts, reduce_first, reduce_second, give_back)
    for number, k in SCHEDULE:
        stages[number](k)

    wait_for(sent.at[0:31], br.at[0])
    landed = back[...].astype(F32).reshape(NS * CAP, W).astype(BF16)
    one = jnp.dot(dt0[...], landed, preferred_element_type=F32)
    two = jnp.dot(dt1[...], landed, preferred_element_type=F32)
    out_ref[...] = (hid[...] + (wcol[:, 2:3] * one + wcol[:, 3:4] * two)).astype(BF16)
    wait_for(hrecv, hs.at[0])
    wait_for(mbuf.at[0:15], ms.at[0])
    for i in range(1, 4):
        wait_for(mbuf, ms.at[i])
    wait_for(gfix.at[0:15], fs.at[0])
    wait_for(gbuf.at[0:15], gs.at[0])
    wait_for(sent.at[0:31], zs.at[0])
    wait_for(sent.at[0:31], bs.at[0])
    for i, size in enumerate((3, 8, 4, 4, 8, 3)):
        wait_for(x_all.at[:, 0 : max(1, size // 4), 0 : min(size, 4)], ss.at[i])


def body(outer_gate, inner_gate, values, conv_taps, document, mix_proj, stream, norm_gain, routes, route_weight, w_gate, w_up, w_down):
    vmem = pl.BlockSpec(memory_space=pltpu.VMEM)
    hbm = pl.BlockSpec(memory_space=pl.ANY)
    dma = pltpu.SemaphoreType.DMA
    scratch = [
        pltpu.VMEM((3, 64, 256), BF16),
        pltpu.VMEM((3, 64), BF16),
        pltpu.VMEM((1, 256), jnp.int32),
        pltpu.VMEM((16, 128), F32),
        pltpu.VMEM((2, 256), jnp.int32),
        pltpu.VMEM((2, 256), F32),
        pltpu.VMEM((64, 2048), BF16),
        pltpu.VMEM((256, W), BF16),
        pltpu.VMEM((2048, 256), BF16),
        pltpu.VMEM((2048, 256), BF16),
        pltpu.VMEM((256, 2048), BF16),
        pltpu.VMEM((72, 128), F32),
        pltpu.VMEM((72, 128), F32),
        pltpu.VMEM((16, 16, W), BF16),
        pltpu.VMEM((3, 16, 16, W), BF16),
        pltpu.VMEM((16, 8, W), BF16),
        pltpu.VMEM((2048, 256), BF16),
        pltpu.VMEM((16, 128, 128), BF16),
        pltpu.VMEM((256, W), F32),
        pltpu.VMEM((NS * CAP, 256), BF16),
        pltpu.VMEM((256, NS * CAP), BF16),
        pltpu.VMEM((256, NS * CAP), BF16),
        pltpu.VMEM((256, 128), F32),
        pltpu.VMEM((NS, CAP, W), BF16),
        pltpu.VMEM((CHUNKS, 4, 4, BLOCKS, CAP, W), BF16),
        pltpu.VMEM((ROWS, 2048), BF16),
        pltpu.VMEM((CHUNKS, 4, 4, BLOCKS, CAP, W), BF16),
        pltpu.VMEM((CHUNKS, 2, 2, 4, PART, CAP, W), BF16),
        pltpu.VMEM((CHUNKS, 2, 2, 4, HALF, CAP, W), BF16),
        pltpu.VMEM((CHUNKS, 2, 3, HALF, CAP, W), BF16),
        pltpu.VMEM((CHUNKS, 2, 4, HALF, CAP, W), BF16),
        pltpu.VMEM((CHUNKS, BLOCKS, CAP, W), BF16),
        pltpu.VMEM((NS, CAP, W), BF16),
        dma((13,)),
        dma((1,)), dma((1,)),
        dma((4,)), dma((4,)),
        dma((1,)), dma((1,)),
        dma((1,)), dma((1,)),
        dma((1,)), dma((CHUNKS,)),
        dma((6,)), dma((6, CHUNKS)),
        dma((1,)), dma((1,)),
    ]
    return pl.pallas_call(
        kernel,
        out_shape=jax.ShapeDtypeStruct((256, W), BF16),
        in_specs=[hbm] * 13,
        out_specs=vmem,
        scratch_shapes=scratch,
        compiler_params=pltpu.CompilerParams(collective_id=0, has_side_effects=True, vmem_limit_bytes=60 * 2**20),
        name="block",
    )(
        outer_gate.T, inner_gate.T, values.T, conv_taps, document.reshape(1, 256), mix_proj, stream, norm_gain.reshape(16, 128),
        routes.T, route_weight.T, w_gate[0], w_up[0], w_down[0],
    )


def solution(mesh):
    placed = (
        P("sp", "tp"), P("sp", "tp"), P("sp", "tp"), P(None, "tp"), P("sp"), P("tp", None), P("sp", None), P(),
        P("sp", None), P("sp", None), P("sp", None, "tp"), P("sp", None, "tp"), P("sp", "tp", None),
    )
    return jax.shard_map(body, mesh=mesh, in_specs=placed, out_specs=P("sp", "tp"), check_vma=False)
```
